32 devices in a mesh: sp: 8 (over z, x), tp: 4 (over y, core).
Axes of the slice: x: 2, y: 2, z: 4, core: 2. Of those that a mesh axis runs over, the one named last changes fastest.
Arguments:
- queries: bfloat16 [4096, 3072], P('sp', 'tp'), may hold values from -6 to 6
- latent: bfloat16 [4096, 1024], P('sp'), may hold values from -6 to 6
- rope_key: bfloat16 [4096, 64], P('sp'), may hold values from -6 to 6
- key_weight: bfloat16 [1024, 2048], P(None, 'tp'), as said below
- value_weight: bfloat16 [1024, 2048], P(None, 'tp'), as said below
- log_sums: float32 [16, 4096], P('tp', 'sp'), as said below
- attn_out: bfloat16 [4096, 2048], P('sp', 'tp'), as said below
- out_grad: bfloat16 [4096, 2048], P('sp', 'tp'), may hold values from -6 to 6
Outputs:
- d_queries: bfloat16 [4096, 3072], P('sp', 'tp')
- d_latent: float32 [4096, 1024], P('sp')
- d_rope: float32 [4096, 64], P('sp')
- d_value_weight: float32 [1024, 2048], P('sp', 'tp')
The draws below stay inside these ranges and needn't reach their ends.
Inputs may be any that keep to these rules, and one draw needn't show every extreme that they name: `key_weight`: independent entries of order one multiplied by 1024^(-1/2). `value_weight`: independent entries of order one multiplied by 1024^(-1/2). log_sums[h, i] is the logarithm of the sum over j <= i of exp(scores[h, i, j]) of the forward pass. attn_out is the forward pass output: head h of row i is the sum over j <= i of exp(scores - log_sums) rounded to bfloat16, times head h of values row j, rounded to bfloat16.
All inputs are finite; a program needn't handle non-finite values.
Results may differ from the reference program's by a relative error of at most 0.018.
Values may be sent and summed in bfloat16 or wider, within the bound.
A program may use at most 192 MiB of HBM per device.

```python
import jax
import jax.numpy as jnp
from jax import lax

HEADS = 16
NOPE = 128
ROPE = 64
VDIM = 128
LATENT = 1024
TOKENS = 4096


def rough_normal(key, shape):
    return jnp.clip(jax.random.normal(key, shape, jnp.float32), -6.0, 6.0)


def base_inputs(key):
    queries = rough_normal(jax.random.fold_in(key, 101), (TOKENS, HEADS * (NOPE + ROPE)))
    latent = rough_normal(jax.random.fold_in(key, 102), (TOKENS, LATENT))
    rope_key = rough_normal(jax.random.fold_in(key, 103), (TOKENS, ROPE))
    key_weight = rough_normal(jax.random.fold_in(key, 104), (LATENT, HEADS * NOPE)) * LATENT ** (-0.5)
    value_weight = rough_normal(jax.random.fold_in(key, 105), (LATENT, HEADS * VDIM)) * LATENT ** (-0.5)
    return (queries.astype(jnp.bfloat16), latent.astype(jnp.bfloat16), rope_key.astype(jnp.bfloat16), key_weight.astype(jnp.bfloat16), value_weight.astype(jnp.bfloat16))


def forward_outputs(key):
    queries, latent, rope_key, key_weight, value_weight = base_inputs(key)
    head_width = NOPE + ROPE
    score_scale = head_width ** (-0.5)
    key_nope = jnp.dot(latent, key_weight, preferred_element_type=jnp.float32).astype(jnp.bfloat16)
    values = jnp.dot(latent, value_weight, preferred_element_type=jnp.float32).astype(jnp.bfloat16)
    query_heads = queries.reshape(TOKENS, HEADS, head_width).transpose(1, 0, 2)
    key_heads = key_nope.reshape(TOKENS, HEADS, NOPE).transpose(1, 0, 2)
    value_heads = values.reshape(TOKENS, HEADS, VDIM).transpose(1, 0, 2)
    positions = jnp.arange(TOKENS, dtype=jnp.int32)
    causal = positions[None, :] <= positions[:, None]

    def one_head(operands):
        query_h, key_h, value_h = operands
        scores = score_scale * (jnp.dot(query_h[:, :NOPE], key_h.T, preferred_element_type=jnp.float32) + jnp.dot(query_h[:, NOPE:], rope_key.T, preferred_element_type=jnp.float32))
        masked = jnp.where(causal, scores, -jnp.inf)
        log_sum = jax.nn.logsumexp(masked, axis=1)
        attn_probs = jnp.exp(masked - log_sum[:, None]).astype(jnp.bfloat16)
        return (log_sum, jnp.dot(attn_probs, value_h, preferred_element_type=jnp.float32).astype(jnp.bfloat16))
    log_sums, out_heads = lax.map(one_head, (query_heads, key_heads, value_heads))
    return (log_sums, out_heads.transpose(1, 0, 2).reshape(TOKENS, HEADS * VDIM))


def draw_queries(key, part):
    return base_inputs(key)[0]


def draw_latent(key, part):
    return base_inputs(key)[1]


def draw_rope_key(key, part):
    return base_inputs(key)[2]


def draw_key_weight(key, part):
    return base_inputs(key)[3]


def draw_value_weight(key, part):
    return base_inputs(key)[4]


def draw_log_sums(key, part):
    return forward_outputs(key)[0]


def draw_attn_out(key, part):
    return forward_outputs(key)[1]


def strengthened(result, key, source, target, shards_of, factor):
    owner, partner = [(jnp.arange(result.shape[dim]) // (result.shape[dim] // shards_of)).reshape([-1 if axis == dim else 1 for axis in range(result.ndim)]) for dim in (source, target)]
    chosen = jax.random.permutation(key, shards_of)[partner]
    strong = (owner == chosen) | (owner == (partner + shards_of // 2) % shards_of)
    return jnp.where(strong, factor * result, result)


def shard_levels(own_key, dims, pieces, low, top_value):
    loudness = 1.0
    for axis_at, blocks in pieces:
        steps = jax.random.uniform(jax.random.fold_in(jax.random.fold_in(own_key, 6), axis_at), (blocks,), jnp.float32, low / len(pieces), top_value / len(pieces))
        loudness = loudness * jnp.repeat(jnp.exp(steps), dims[axis_at] // blocks).reshape((-1,) + (1,) * (len(dims) - 1 - axis_at))
    return loudness


def noise_with(rng, extent, deviation, reach, split, heavy, kind=jnp.bfloat16):
    drawn = deviation * jax.random.normal(rng, extent, jnp.float32)
    if split:
        drawn = drawn * shard_levels(rng, extent, split, -0.22, 0.18)
    return jnp.clip(strengthened(drawn, jax.random.fold_in(rng, 3), *heavy), -reach, reach).astype(kind)


def setup_inputs(seed: int = 0) -> dict:
    keys = jax.random.split(jax.random.key(seed), 9)
    return {
        "queries": draw_queries(jax.random.fold_in(keys[8], 71), 0),
        "latent": draw_latent(jax.random.fold_in(keys[8], 71), 0),
        "rope_key": draw_rope_key(jax.random.fold_in(keys[8], 71), 0),
        "key_weight": draw_key_weight(jax.random.fold_in(keys[8], 71), 0),
        "value_weight": draw_value_weight(jax.random.fold_in(keys[8], 71), 0),
        "log_sums": draw_log_sums(jax.random.fold_in(keys[8], 71), 0),
        "attn_out": draw_attn_out(jax.random.fold_in(keys[8], 71), 0),
        "out_grad": noise_with(keys[7], (TOKENS, HEADS * VDIM), 1.0, 6.0, ((0, 8), (1, 4)), (0, 1, 8, 2.0)),
    }


def reference(queries, latent, rope_key, key_weight, value_weight, log_sums, attn_out, out_grad):
    tok_count = queries.shape[0]
    head_width = NOPE + ROPE
    score_scale = head_width ** -0.5
    key_nope = jnp.dot(latent, key_weight, preferred_element_type=jnp.float32).astype(jnp.bfloat16)
    values = jnp.dot(latent, value_weight, preferred_element_type=jnp.float32).astype(jnp.bfloat16)
    query_heads = queries.reshape(tok_count, HEADS, head_width).transpose(1, 0, 2)
    key_heads = key_nope.reshape(tok_count, HEADS, NOPE).transpose(1, 0, 2)
    value_heads = values.reshape(tok_count, HEADS, VDIM).transpose(1, 0, 2)
    grad_heads = out_grad.reshape(tok_count, HEADS, VDIM).transpose(1, 0, 2)
    out_heads = attn_out.reshape(tok_count, HEADS, VDIM).transpose(1, 0, 2)
    row_terms = jnp.sum(out_heads.astype(jnp.float32) * grad_heads.astype(jnp.float32), axis=-1)
    positions = jnp.arange(tok_count, dtype=jnp.int32)
    causal = positions[None, :] <= positions[:, None]

    def one_head(operands):
        query_h, key_h, value_h, grad_h, lse_h, delta_h = operands
        scores = score_scale * (jnp.dot(query_h[:, :NOPE], key_h.T, preferred_element_type=jnp.float32)
                                + jnp.dot(query_h[:, NOPE:], rope_key.T, preferred_element_type=jnp.float32))
        attn_probs = jnp.exp(jnp.where(causal, scores - lse_h[:, None], -1e30))
        probs_b = attn_probs.astype(jnp.bfloat16)
        value_grad = jnp.dot(probs_b.T, grad_h, preferred_element_type=jnp.float32)
        prob_grad = jnp.dot(grad_h, value_h.T, preferred_element_type=jnp.float32)
        score_grad = (attn_probs * (prob_grad - delta_h[:, None])).astype(jnp.bfloat16)
        query_grad = score_scale * jnp.concatenate(
            [jnp.dot(score_grad, key_h, preferred_element_type=jnp.float32),
             jnp.dot(score_grad, rope_key, preferred_element_type=jnp.float32)], axis=1)
        key_grad = score_scale * jnp.dot(score_grad.T, query_h[:, :NOPE], preferred_element_type=jnp.float32)
        rope_grad = score_scale * jnp.dot(score_grad.T, query_h[:, NOPE:], preferred_element_type=jnp.float32)
        return query_grad, key_grad, rope_grad, value_grad

    query_grad, key_grad, rope_grad, value_grad = lax.map(
        one_head, (query_heads, key_heads, value_heads, grad_heads, log_sums, row_terms))
    d_queries = query_grad.transpose(1, 0, 2).reshape(tok_count, HEADS * head_width).astype(jnp.bfloat16)
    key_grad_b = key_grad.transpose(1, 0, 2).reshape(tok_count, HEADS * NOPE).astype(jnp.bfloat16)
    value_grad_b = value_grad.transpose(1, 0, 2).reshape(tok_count, HEADS * VDIM).astype(jnp.bfloat16)
    d_latent = (jnp.dot(key_grad_b, key_weight.T, preferred_element_type=jnp.float32)
                + jnp.dot(value_grad_b, value_weight.T, preferred_element_type=jnp.float32))
    d_rope = jnp.sum(rope_grad, axis=0)
    d_value_weight = jnp.dot(latent.T, value_grad_b, preferred_element_type=jnp.float32)
    return (d_queries, d_latent, d_rope, d_value_weight)
```

```python
import functools

import jax
import jax.numpy as jnp
from jax import lax
from jax.experimental import pallas as pl
from jax.experimental.pallas import tpu as pltpu
from jax.sharding import PartitionSpec as P

NOPE = 128
ROPE = 64
VDIM = 128
WIDE = 256
LOG2E = 1.4426950408889634
BF16 = jnp.bfloat16
F32 = jnp.float32


def dot_nn(a, b):
    return lax.dot_general(a, b, (((1,), (0,)), ((), ())), preferred_element_type=F32)


def dot_nt(a, b):
    return lax.dot_general(a, b, (((1,), (1,)), ((), ())), preferred_element_type=F32)


def attn_kernel(
    heads,
    latent_dim,
    mine_ref,
    q_ref,
    g_ref,
    lse_ref,
    delta_ref,
    lat_ref,
    wk_ref,
    wv_ref,
    dq_ref,
    dlat_ref,
    dvw_ref,
    q_s,
    qt_s,
    gt_s,
    dqt_s,
    kc_s,
    kct_s,
    v_s,
    dk_s,
    dv_s,
):
    j = pl.program_id(0)
    mine = mine_ref[0]
    rows = q_ref.shape[0]
    width = NOPE + ROPE
    scale = width ** (-0.5)

    @pl.when(j == 0)
    def _():
        for h in range(heads):
            qh = jnp.concatenate(
                [q_ref[:, h * width : (h + 1) * width], jnp.zeros((rows, WIDE - width), BF16)],
                axis=1,
            )
            q_s[h] = qh
            qt_s[h] = qh.T
            gt_s[h] = g_ref[:, h * VDIM : (h + 1) * VDIM].T
        dqt_s[...] = jnp.zeros_like(dqt_s)
        dvw_ref[...] = jnp.zeros_like(dvw_ref)

    @pl.when(j > mine)
    def _():
        dlat_ref[...] = jnp.zeros_like(dlat_ref)

    @pl.when(j <= mine)
    def _():
        lat = lat_ref[:, :latent_dim]
        rope = lat_ref[:, latent_dim:]
        keys = dot_nn(lat, wk_ref[...]).astype(BF16)
        v_s[...] = dot_nn(lat, wv_ref[...]).astype(BF16)
        for h in range(heads):
            kc = jnp.concatenate([keys[:, h * NOPE : (h + 1) * NOPE], rope], axis=1)
            kc_s[h] = kc
            kct_s[h] = kc.T
        rope_sum = jnp.zeros((rows, WIDE - NOPE), F32)
        k_pos = lax.broadcasted_iota(jnp.int32, (rows, rows), 0)
        q_pos = lax.broadcasted_iota(jnp.int32, (rows, rows), 1)
        causal = k_pos - q_pos <= (mine - j) * rows
        for h in range(heads):
            s = dot_nn(kc_s[h], qt_s[h])
            z = s * (scale * LOG2E) - lse_ref[h : h + 1, :] * LOG2E
            p = jnp.exp2(jnp.where(causal, z, -1e30))
            dp = dot_nn(v_s[:, h * VDIM : (h + 1) * VDIM], gt_s[h])
            ds = (p * (dp - delta_ref[h : h + 1, :])).astype(BF16)
            dv_s[:, h * VDIM : (h + 1) * VDIM] = dot_nn(
                p.astype(BF16), g_ref[:, h * VDIM : (h + 1) * VDIM]
            ).astype(BF16)
            dk = scale * dot_nn(ds, q_s[h])
            dk_s[:, h * NOPE : (h + 1) * NOPE] = dk[:, :NOPE].astype(BF16)
            rope_sum = rope_sum + dk[:, NOPE:]
            dqt_s[h] += dot_nn(kct_s[h], ds)
        dlat = dot_nt(dk_s[...], wk_ref[...]) + dot_nt(dv_s[...], wv_ref[...])
        dlat_ref[:, :latent_dim] = dlat.astype(BF16)
        dlat_ref[:, latent_dim:] = rope_sum.astype(BF16)
        dvw_ref[...] += dot_nn(lat.T, dv_s[...])

    @pl.when(j == pl.num_programs(0) - 1)
    def _():
        for h in range(heads):
            dq_ref[:, h * width : (h + 1) * width] = (
                (scale * dqt_s[h]).T[:, :width].astype(BF16)
            )


def attn_backward(mine, queries, out_grad, lse, delta, lat_all, key_weight, value_weight):
    rows = queries.shape[0]
    latent_dim = key_weight.shape[0]
    heads = key_weight.shape[1] // NOPE
    blocks = lat_all.shape[0] // rows
    packed = lat_all.shape[1]

    def whole(j, m):
        return (0, 0)

    return pl.pallas_call(
        functools.partial(attn_kernel, heads, latent_dim),
        grid_spec=pltpu.PrefetchScalarGridSpec(
            num_scalar_prefetch=1,
            grid=(blocks,),
            in_specs=[
                pl.BlockSpec(queries.shape, whole),
                pl.BlockSpec(out_grad.shape, whole),
                pl.BlockSpec(lse.shape, whole),
                pl.BlockSpec(delta.shape, whole),
                pl.BlockSpec((rows, packed), lambda j, m: (jnp.minimum(j, m[0]), 0)),
                pl.BlockSpec(key_weight.shape, whole),
                pl.BlockSpec(value_weight.shape, whole),
            ],
            out_specs=[
                pl.BlockSpec(queries.shape, whole),
                pl.BlockSpec((rows, packed), lambda j, m: (j, 0)),
                pl.BlockSpec(value_weight.shape, whole),
            ],
            scratch_shapes=[
                pltpu.VMEM((heads, rows, WIDE), BF16),
                pltpu.VMEM((heads, WIDE, rows), BF16),
                pltpu.VMEM((heads, VDIM, rows), BF16),
                pltpu.VMEM((heads, WIDE, rows), F32),
                pltpu.VMEM((heads, rows, WIDE), BF16),
                pltpu.VMEM((heads, WIDE, rows), BF16),
                pltpu.VMEM((rows, heads * VDIM), BF16),
                pltpu.VMEM((rows, heads * NOPE), BF16),
                pltpu.VMEM((rows, heads * VDIM), BF16),
            ],
        ),
        out_shape=[
            jax.ShapeDtypeStruct(queries.shape, BF16),
            jax.ShapeDtypeStruct(lat_all.shape, BF16),
            jax.ShapeDtypeStruct(value_weight.shape, F32),
        ],
        compiler_params=pltpu.CompilerParams(
            dimension_semantics=("arbitrary",), vmem_limit_bytes=60 * 1024 * 1024
        ),
    )(mine, queries, out_grad, lse, delta, lat_all, key_weight, value_weight)


def per_device(queries, latent, rope_key, key_weight, value_weight, log_sums, attn_out, out_grad):
    rows, latent_dim = latent.shape
    heads = key_weight.shape[1] // NOPE
    tp = lax.axis_size("tp")
    mine = lax.axis_index("sp").astype(jnp.int32).reshape((1,))
    row_terms = jnp.sum(
        attn_out.reshape(rows, heads, VDIM).astype(F32)
        * out_grad.reshape(rows, heads, VDIM).astype(F32),
        axis=2,
    ).T
    part = rows // tp
    start = lax.axis_index("tp") * part
    lat_piece = lax.dynamic_slice_in_dim(latent, start, part, 0)
    rope_piece = lax.dynamic_slice_in_dim(rope_key, start, part, 0)
    piece = jnp.concatenate(
        [lat_piece, rope_piece, jnp.zeros((part, WIDE - NOPE - ROPE), BF16)], axis=1
    )
    lat_all = lax.all_gather(piece, ("sp", "tp"), axis=0, tiled=True)
    d_queries, dlat, dvw = attn_backward(
        mine, queries, out_grad, log_sums, row_terms, lat_all, key_weight, value_weight
    )
    dlat_piece = lax.psum_scatter(dlat, ("sp", "tp"), scatter_dimension=0, tiled=True)
    d_value_weight = lax.psum_scatter(
        dvw.astype(BF16), "sp", scatter_dimension=0, tiled=True
    ).astype(F32)
    dlat_own = lax.all_gather(dlat_piece, "tp", axis=0, tiled=True)
    d_latent = dlat_own[:, :latent_dim].astype(F32)
    d_rope = dlat_own[:, latent_dim : latent_dim + ROPE].astype(F32)
    return (d_queries, d_latent, d_rope, d_value_weight)


def solution(mesh):
    placed = (
        P("sp", "tp"),
        P("sp", None),
        P("sp", None),
        P(None, "tp"),
        P(None, "tp"),
        P("tp", "sp"),
        P("sp", "tp"),
        P("sp", "tp"),
    )
    return jax.shard_map(
        per_device,
        mesh=mesh,
        in_specs=placed,
        out_specs=(P("sp", "tp"), P("sp", None), P("sp", None), P("sp", "tp")),
        check_vma=False,
    )
```

```python
import functools

import jax
import jax.numpy as jnp
from jax import lax
from jax.experimental import pallas as pl
from jax.experimental.pallas import tpu as pltpu
from jax.sharding import PartitionSpec as P

NOPE = 128
ROPE = 64
VDIM = 128
WIDE = 256
LOG2E = 1.4426950408889634
BF16 = jnp.bfloat16
F32 = jnp.float32


def dot_nn(a, b):
    return lax.dot_general(a, b, (((1,), (0,)), ((), ())), preferred_element_type=F32)


def dot_nt(a, b):
    return lax.dot_general(a, b, (((1,), (1,)), ((), ())), preferred_element_type=F32)


def attn_kernel(
    heads,
    latent_dim,
    mine_ref,
    q_ref,
    g_ref,
    lse_ref,
    delta_ref,
    lat_ref,
    wk_ref,
    wv_ref,
    dq_ref,
    dlat_ref,
    dvw_ref,
    q_s,
    qt_s,
    gt_s,
    dqt_s,
    kc_s,
    kct_s,
    v_s,
    dk_s,
    dv_s,
):
    j = pl.program_id(0)
    mine = mine_ref[0]
    rows = q_ref.shape[0]
    width = NOPE + ROPE
    scale = width ** (-0.5)

    @pl.when(j == 0)
    def _():
        for h in range(heads):
            qh = jnp.concatenate(
                [q_ref[:, h * width : (h + 1) * width], jnp.zeros((rows, WIDE - width), BF16)],
                axis=1,
            )
            q_s[h] = qh
            qt_s[h] = qh.T
            gt_s[h] = g_ref[:, h * VDIM : (h + 1) * VDIM].T
        dqt_s[...] = jnp.zeros_like(dqt_s)
        dvw_ref[...] = jnp.zeros_like(dvw_ref)

    @pl.when(j > mine)
    def _():
        dlat_ref[...] = jnp.zeros_like(dlat_ref)

    @pl.when(j <= mine)
    def _():
        lat = lat_ref[:, :latent_dim]
        rope = lat_ref[:, latent_dim:]
        keys = dot_nn(lat, wk_ref[...]).astype(BF16)
        v_s[...] = dot_nn(lat, wv_ref[...]).astype(BF16)
        for h in range(heads):
            kc = jnp.concatenate([keys[:, h * NOPE : (h + 1) * NOPE], rope], axis=1)
            kc_s[h] = kc
            kct_s[h] = kc.T
        rope_sum = jnp.zeros((rows, WIDE - NOPE), F32)
        k_pos = lax.broadcasted_iota(jnp.int32, (rows, rows), 0)
        q_pos = lax.broadcasted_iota(jnp.int32, (rows, rows), 1)
        causal = k_pos - q_pos <= (mine - j) * rows
        for h in range(heads):
            s = dot_nn(kc_s[h], qt_s[h])
            z = s * (scale * LOG2E) - lse_ref[h : h + 1, :] * LOG2E
            p = jnp.exp2(jnp.where(causal, z, -1e30))
            dp = dot_nn(v_s[:, h * VDIM : (h + 1) * VDIM], gt_s[h])
            ds = (p * (dp - delta_ref[h : h + 1, :])).astype(BF16)
            dv_s[:, h * VDIM : (h + 1) * VDIM] = dot_nn(
                p.astype(BF16), g_ref[:, h * VDIM : (h + 1) * VDIM]
            ).astype(BF16)
            dk = scale * dot_nn(ds, q_s[h])
            dk_s[:, h * NOPE : (h + 1) * NOPE] = dk[:, :NOPE].astype(BF16)
            rope_sum = rope_sum + dk[:, NOPE:]
            dqt_s[h] += dot_nn(kct_s[h], ds)
        dlat = dot_nt(dk_s[...], wk_ref[...]) + dot_nt(dv_s[...], wv_ref[...])
        dlat_ref[:, :latent_dim] = dlat.astype(BF16)
        dlat_ref[:, latent_dim:] = rope_sum.astype(BF16)
        dvw_ref[...] += dot_nn(lat.T, dv_s[...])

    @pl.when(j == pl.num_programs(0) - 1)
    def _():
        for h in range(heads):
            dq_ref[:, h * width : (h + 1) * width] = (
                (scale * dqt_s[h]).T[:, :width].astype(BF16)
            )


def attn_backward(mine, queries, out_grad, lse, delta, lat_all, key_weight, value_weight):
    rows = queries.shape[0]
    latent_dim = key_weight.shape[0]
    heads = key_weight.shape[1] // NOPE
    blocks = lat_all.shape[0] // rows
    packed = lat_all.shape[1]

    def whole(j, m):
        return (0, 0)

    return pl.pallas_call(
        functools.partial(attn_kernel, heads, latent_dim),
        grid_spec=pltpu.PrefetchScalarGridSpec(
            num_scalar_prefetch=1,
            grid=(blocks,),
            in_specs=[
                pl.BlockSpec(queries.shape, whole),
                pl.BlockSpec(out_grad.shape, whole),
                pl.BlockSpec(lse.shape, whole),
                pl.BlockSpec(delta.shape, whole),
                pl.BlockSpec((rows, packed), lambda j, m: (jnp.minimum(j, m[0]), 0)),
                pl.BlockSpec(key_weight.shape, whole),
                pl.BlockSpec(value_weight.shape, whole),
            ],
            out_specs=[
                pl.BlockSpec(queries.shape, whole),
                pl.BlockSpec((rows, packed), lambda j, m: (j, 0)),
                pl.BlockSpec(value_weight.shape, whole),
            ],
            scratch_shapes=[
                pltpu.VMEM((heads, rows, WIDE), BF16),
                pltpu.VMEM((heads, WIDE, rows), BF16),
                pltpu.VMEM((heads, VDIM, rows), BF16),
                pltpu.VMEM((heads, WIDE, rows), F32),
                pltpu.VMEM((heads, rows, WIDE), BF16),
                pltpu.VMEM((heads, WIDE, rows), BF16),
                pltpu.VMEM((rows, heads * VDIM), BF16),
                pltpu.VMEM((rows, heads * NOPE), BF16),
                pltpu.VMEM((rows, heads * VDIM), BF16),
            ],
        ),
        out_shape=[
            jax.ShapeDtypeStruct(queries.shape, BF16),
            jax.ShapeDtypeStruct(lat_all.shape, BF16),
            jax.ShapeDtypeStruct(value_weight.shape, F32),
        ],
        compiler_params=pltpu.CompilerParams(
            dimension_semantics=("arbitrary",), vmem_limit_bytes=60 * 1024 * 1024
        ),
    )(mine, queries, out_grad, lse, delta, lat_all, key_weight, value_weight)


def per_device(queries, latent, rope_key, key_weight, value_weight, log_sums, attn_out, out_grad):
    rows, latent_dim = latent.shape
    heads = key_weight.shape[1] // NOPE
    tp = lax.axis_size("tp")
    mine = lax.axis_index("sp").astype(jnp.int32).reshape((1,))
    row_terms = jnp.sum(
        attn_out.reshape(rows, heads, VDIM).astype(F32)
        * out_grad.reshape(rows, heads, VDIM).astype(F32),
        axis=2,
    ).T
    part = rows // tp
    start = lax.axis_index("tp") * part
    lat_piece = lax.dynamic_slice_in_dim(latent, start, part, 0)
    rope_piece = lax.dynamic_slice_in_dim(rope_key, start, part, 0)
    piece = jnp.concatenate(
        [lat_piece, rope_piece, jnp.zeros((part, WIDE - NOPE - ROPE), BF16)], axis=1
    )
    lat_all = lax.all_gather(piece, ("sp", "tp"), axis=0, tiled=True)
    d_queries, dlat, dvw = attn_backward(
        mine, queries, out_grad, log_sums, row_terms, lat_all, key_weight, value_weight
    )
    dlat_piece = lax.psum_scatter(dlat, ("sp", "tp"), scatter_dimension=0, tiled=True)
    sp = lax.axis_size("sp")
    dvw_parts = lax.all_to_all(dvw.astype(BF16), "sp", 0, 0, tiled=True)
    d_value_weight = jnp.sum(
        dvw_parts.reshape(sp, latent_dim // sp, dvw.shape[1]).astype(F32), axis=0
    )
    dlat_own = lax.all_gather(dlat_piece, "tp", axis=0, tiled=True)
    d_latent = dlat_own[:, :latent_dim].astype(F32)
    d_rope = dlat_own[:, latent_dim : latent_dim + ROPE].astype(F32)
    return (d_queries, d_latent, d_rope, d_value_weight)


def solution(mesh):
    placed = (
        P("sp", "tp"),
        P("sp", None),
        P("sp", None),
        P(None, "tp"),
        P(None, "tp"),
        P("tp", "sp"),
        P("sp", "tp"),
        P("sp", "tp"),
    )
    return jax.shard_map(
        per_device,
        mesh=mesh,
        in_specs=placed,
        out_specs=(P("sp", "tp"), P("sp", None), P("sp", None), P("sp", "tp")),
        check_vma=False,
    )
```
